32 devices in a mesh: sp: 16 (over z, y, x), tp: 2 (over core).
Axes of the slice: x: 2, y: 2, z: 4, core: 2. Of those that a mesh axis runs over, the one named last changes fastest.
Arguments:
- stream: bfloat16 [4096, 2048], P(('sp', 'tp')), may hold values from -6 to 6
- queries: bfloat16 [4096, 1024], P('sp', 'tp'), may hold values from -6 to 6
- keys_in: bfloat16 [4096, 1024], P('sp', 'tp'), may hold values from -6 to 6
- values_in: bfloat16 [4096, 1024], P('sp', 'tp'), may hold values from -6 to 6
- gate_in: bfloat16 [4096, 1024], P('sp', 'tp'), may hold values from -6 to 6
- log_decay: float32 [4096, 8], P('sp', 'tp'), may hold values from -0.8 to 0
- head_gain: bfloat16 [1024], P('tp'), may hold values from 0.099609375 to 1.8984375
- out_weight: bfloat16 [1024, 2048], P('tp'), may hold values from -0.1875 to 0.1875
- norm_gain: bfloat16 [2048], replicated, may hold values from 0.099609375 to 1.8984375
- gate_weight: bfloat16 [2048, 5632], P('sp', 'tp'), may hold values from -0.125 to 0.125
- up_weight: bfloat16 [2048, 5632], P('sp', 'tp'), may hold values from -0.125 to 0.125
- down_weight: bfloat16 [5632, 2048], P('tp', 'sp'), may hold values from -0.078125 to 0.078125
Outputs:
- result: bfloat16 [4096, 2048], P(('sp', 'tp'))
The draws below stay inside these ranges and needn't reach their ends.
All inputs are finite; a program needn't handle non-finite values.
Results may differ from the reference program's by a relative error of at most 0.02.
Values may be sent and summed in bfloat16 or wider, within the bound.
A program may use at most 128 MiB of HBM per device.

```python
import jax
import jax.numpy as jnp
from jax import lax

D = 2048
HEAD_COUNT = 8
HEAD_DIM = 128
FF = 5632
BLOCK = 128
TOK_DEV = 256
TOKEN_COUNT = 4096
N_TP = 2


def draw_log_decay(key, part):
    draw_keys = jax.random.split(jax.random.fold_in(key, 11), 7)
    is_fast = jax.random.randint(draw_keys[0], (HEAD_COUNT,), 0, 2) == 0
    slow_rate = jax.random.uniform(draw_keys[1], (HEAD_COUNT,), jnp.float32, 0.2, 0.6) / TOKEN_COUNT
    fast_rate = 1.0 / jax.random.uniform(draw_keys[2], (HEAD_COUNT,), jnp.float32, 30.0, 100.0)
    head_rate = jnp.where(is_fast, fast_rate, slow_rate)
    block_count = TOKEN_COUNT // TOK_DEV
    block_factor = jax.random.uniform(draw_keys[3], (block_count, 1, HEAD_COUNT), jnp.float32, 0.4, 1.6)
    roughness = jax.random.uniform(draw_keys[4], (block_count, TOK_DEV, HEAD_COUNT), jnp.float32, 0.5, 1.5)
    drawn_reference = -(head_rate * block_factor * roughness).reshape(TOKEN_COUNT, HEAD_COUNT)
    spike_locations = jax.random.randint(draw_keys[5], (2, HEAD_COUNT), 0, TOKEN_COUNT)
    spike_drops = jnp.log(jax.random.uniform(draw_keys[6], (2, HEAD_COUNT), jnp.float32, 0.5, 0.8))
    token_positions = jnp.arange(TOKEN_COUNT)[:, None]
    spike_events = jnp.sum(jnp.where(token_positions[None] == spike_locations[:, None, :], spike_drops[:, None, :], 0.0), axis=0)
    return drawn_reference + spike_events


def level_of(own_key, extent, cuts, smallest, largest):
    level = 1.0
    for position, blocks in cuts:
        heights = jax.random.uniform(jax.random.fold_in(jax.random.fold_in(own_key, 6), position), (blocks,), jnp.float32, smallest / len(cuts), largest / len(cuts))
        level = level * jnp.repeat(jnp.exp(heights), extent[position] // blocks).reshape((-1,) + (1,) * (len(extent) - 1 - position))
    return level


def centred(own_key, extent, scale, bound, cuts=(), held_as=jnp.bfloat16):
    drawn = scale * jax.random.normal(own_key, extent, jnp.float32)
    if cuts:
        drawn = drawn * level_of(own_key, extent, cuts, -0.22, 0.18)
    return jnp.clip(drawn, -bound, bound).astype(held_as)


def setup_inputs(seed: int = 0) -> dict:
    streams_of = jax.random.split(jax.random.key(seed), 13)
    return {
        "stream": centred(streams_of[0], (TOKEN_COUNT, D), 0.7, 6.0, ((0, 32),)),
        "queries": centred(streams_of[1], (TOKEN_COUNT, HEAD_COUNT * HEAD_DIM), 1.0, 6.0, ((0, 16), (1, 2))),
        "keys_in": centred(streams_of[2], (TOKEN_COUNT, HEAD_COUNT * HEAD_DIM), 1.0, 6.0, ((0, 16), (1, 2))),
        "values_in": centred(streams_of[3], (TOKEN_COUNT, HEAD_COUNT * HEAD_DIM), 1.0, 6.0, ((0, 16), (1, 2))),
        "gate_in": centred(streams_of[4], (TOKEN_COUNT, HEAD_COUNT * HEAD_DIM), 1.0, 6.0, ((0, 16), (1, 2))),
        "log_decay": draw_log_decay(jax.random.fold_in(streams_of[12], 71), 0),
        "head_gain": jnp.clip(1.0 + 0.18 * jax.random.normal(streams_of[6], (HEAD_COUNT * HEAD_DIM,), jnp.float32), 0.099609375, 1.8984375).astype(jnp.bfloat16),
        "out_weight": centred(streams_of[7], (HEAD_COUNT * HEAD_DIM, D), (HEAD_COUNT * HEAD_DIM) ** -0.5, 0.1875, ((0, 2),)),
        "norm_gain": jnp.clip(1.0 + 0.18 * jax.random.normal(streams_of[8], (D,), jnp.float32), 0.099609375, 1.8984375).astype(jnp.bfloat16),
        "gate_weight": centred(streams_of[9], (D, FF), D ** -0.5, 0.125, ((0, 16), (1, 2))),
        "up_weight": centred(streams_of[10], (D, FF), D ** -0.5, 0.125, ((0, 16), (1, 2))),
        "down_weight": centred(streams_of[11], (FF, D), FF ** -0.5, 0.078125, ((0, 2), (1, 16))),
    }


epsilon = 1e-06
highest = lax.Precision.HIGHEST

def block_pass(state, block_inputs):
    query_block, key_block, value_block, decay_block = block_inputs
    head_dim = query_block.shape[-1]
    key_scale = head_dim ** (-0.5)
    running = jnp.cumsum(decay_block, axis=0)
    query_wide = query_block.astype(jnp.float32)
    key_plain = key_block.astype(jnp.float32)
    value_wide = value_block.astype(jnp.float32)
    scores = jnp.einsum('ihd,jhd->hij', query_wide, key_plain, precision=highest) * key_scale
    offsets = jnp.arange(decay_block.shape[0])
    causal = offsets[:, None] >= offsets[None, :]
    log_gap = running.T[:, :, None] - running.T[:, None, :]
    decay_table = jnp.where(causal[None], jnp.exp(jnp.minimum(log_gap, 0.0)), 0.0)
    within = jnp.einsum('hij,jhe->ihe', scores * decay_table, value_wide, precision=highest)
    carried = jnp.einsum('ihd,hde->ihe', query_wide * jnp.exp(running)[:, :, None], state, precision=highest)
    block_total = running[-1]
    key_wide = key_plain * key_scale * jnp.exp(block_total[None] - running)[:, :, None]
    state = jnp.exp(block_total)[:, None, None] * state + jnp.einsum('jhd,jhe->hde', key_wide, value_wide, precision=highest)
    return (state, within + carried)

def reference(stream, queries, keys_in, values_in, gate_in, log_decay, head_gain, out_weight, norm_gain, gate_weight, up_weight, down_weight):
    heads = log_decay.shape[1]
    head_dim = queries.shape[1] // heads
    block_count = TOKEN_COUNT // BLOCK
    block_shape = (block_count, BLOCK, heads, head_dim)
    block_inputs = (queries.reshape(block_shape), keys_in.reshape(block_shape), values_in.reshape(block_shape), log_decay.reshape(block_count, BLOCK, heads))
    start_state = jnp.zeros((heads, head_dim, head_dim), jnp.float32)
    final_state, retained = lax.scan(block_pass, start_state, block_inputs)
    retained = retained.reshape(TOKEN_COUNT, heads, head_dim)
    center = lax.optimization_barrier(jnp.mean(retained, axis=-1, keepdims=True))
    spread = lax.optimization_barrier(jnp.mean(jnp.square(retained - center), axis=-1, keepdims=True))
    normed_heads = (retained - center) * lax.rsqrt(spread + epsilon) * head_gain.astype(jnp.float32).reshape(heads, head_dim)
    mixed = (jax.nn.silu(gate_in.astype(jnp.float32)) * normed_heads.reshape(TOKEN_COUNT, heads * head_dim)).astype(jnp.bfloat16)
    group_width = heads * head_dim // N_TP
    attended = jnp.zeros((TOKEN_COUNT, D), jnp.float32)
    for group_index in range(N_TP):
        lo_col = group_index * group_width
        group_term = jnp.dot(mixed[:, lo_col:lo_col + group_width], out_weight[lo_col:lo_col + group_width], preferred_element_type=jnp.float32)
        attended = attended + lax.optimization_barrier(group_term.astype(jnp.bfloat16)).astype(jnp.float32)
    residual = stream.astype(jnp.float32) + attended
    normed = (residual * lax.rsqrt(lax.optimization_barrier(jnp.mean(residual * residual, axis=-1, keepdims=True)) + epsilon) * norm_gain.astype(jnp.float32)).astype(jnp.bfloat16)
    gate_sum = jnp.dot(normed, gate_weight, preferred_element_type=jnp.float32)
    up_sum = jnp.dot(normed, up_weight, preferred_element_type=jnp.float32)
    hidden = (jax.nn.silu(gate_sum) * up_sum).astype(jnp.bfloat16)
    unit_width = FF // N_TP
    mixer_out = jnp.zeros((TOKEN_COUNT, D), jnp.float32)
    for group_index in range(N_TP):
        lo_unit = group_index * unit_width
        group_term = jnp.dot(hidden[:, lo_unit:lo_unit + unit_width], down_weight[lo_unit:lo_unit + unit_width], preferred_element_type=jnp.float32)
        mixer_out = mixer_out + lax.optimization_barrier(group_term.astype(jnp.bfloat16)).astype(jnp.float32)
    return (residual + mixer_out).astype(jnp.bfloat16)
```

```python
import jax
import jax.numpy as jnp
from jax import lax
from jax.sharding import Mesh, PartitionSpec as P

epsilon = 1e-06
GROUP = 4
SP = ("far", "near")
f32, bf16 = jnp.float32, jnp.bfloat16


def swap(value, axis, bits):
    size = lax.axis_size(axis)
    return lax.ppermute(value, axis, [(i, i ^ bits) for i in range(size)])


def gather_near(value):
    size = lax.axis_size("near")
    if size != 4:
        return {0: value, **{s: swap(value, "near", s) for s in range(1, size)}}
    one, two = swap(value, "near", 1), swap(value, "near", 2)
    half = value.shape[0] // 2
    three = jnp.concatenate(
        [swap(one[:half], "near", 2), swap(two[half:], "near", 1)], axis=0
    )
    return {0: value, 1: one, 2: two, 3: three}


def spread_weights(gate_weight, up_weight, down_weight):
    groups, near = lax.axis_size("far"), lax.axis_size("near")
    far_at, near_at = lax.axis_index("far"), lax.axis_index("near")
    depth, units = gate_weight.shape
    width = units // groups
    total = groups * near
    gate_full = jnp.zeros((depth * total, width), bf16)
    up_full = jnp.zeros((depth * total, width), bf16)
    down_full = jnp.zeros((width, down_weight.shape[1] * total), bf16)
    pieces = []
    for s in range(groups):
        at = (far_at ^ s) * width
        rows = jnp.concatenate(
            [
                lax.dynamic_slice_in_dim(gate_weight, at, width, 1),
                lax.dynamic_slice_in_dim(up_weight, at, width, 1),
            ],
            axis=0,
        )
        columns = lax.dynamic_slice_in_dim(down_weight, at, width, 0)
        if s:
            rows, columns = swap(rows, "far", s), swap(columns, "far", s)
        pieces.append((rows, columns))
    for s, (rows, columns) in enumerate(pieces):
        all_rows, all_columns = gather_near(rows), gather_near(columns)
        for t in range(near):
            at = ((far_at ^ s) * near + (near_at ^ t)) * depth
            gate_full = lax.dynamic_update_slice_in_dim(gate_full, all_rows[t][:depth], at, 0)
            up_full = lax.dynamic_update_slice_in_dim(up_full, all_rows[t][depth:], at, 0)
            down_full = lax.dynamic_update_slice_in_dim(down_full, all_columns[t], at, 1)
    return gate_full, up_full, down_full


def gather_pair(rows):
    if lax.axis_size("tp") == 2:
        return jnp.concatenate([rows, swap(rows, "tp", 1)], axis=0)
    return lax.all_gather(rows, "tp", axis=0, tiled=True)


def scatter_pair(terms):
    terms = terms.astype(bf16)
    if lax.axis_size("tp") == 2:
        half = terms.shape[0] // 2
        return terms[:half].astype(f32) + swap(terms[half:], "tp", 1).astype(f32)
    return lax.psum_scatter(terms, "tp", scatter_dimension=0, tiled=True).astype(f32)


def dot(a, b, dims=((1,), (0,))):
    return lax.dot_general(a, b, (dims, ((), ())), preferred_element_type=f32)


def retention(queries, keys_in, values_in, log_decay):
    row_count, heads = log_decay.shape
    dim = queries.shape[1] // heads
    scale = dim ** (-0.5)
    running = jnp.cumsum(log_decay, axis=0)
    total = running[-1]
    offsets = jnp.arange(row_count)
    causal = offsets[:, None] >= offsets[None, :]
    within, states = [], []
    for h in range(heads):
        cut = slice(h * dim, (h + 1) * dim)
        q, k, v = queries[:, cut], keys_in[:, cut], values_in[:, cut]
        col = running[:, h]
        gap = jnp.minimum(col[:, None] - col[None, :], 0.0)
        table = jnp.where(causal, jnp.exp(gap), 0.0) * scale
        within.append(dot((dot(q, k, ((1,), (1,))) * table).astype(bf16), v))
        tail = (jnp.exp(total[h] - col) * scale)[:, None]
        states.append(dot((k.astype(f32) * tail).astype(bf16), v, ((0,), (0,))))
    return running, total, within, jnp.concatenate(states, axis=0)


def incoming_states(total, state):
    heads = total.shape[0]
    near = lax.axis_size("near")
    here = lax.axis_index("far") * near + lax.axis_index("near")
    high = lax.reduce_precision(total, 8, 7)
    mid = lax.reduce_precision(total - high, 8, 7)
    low = total - high - mid
    parts = jnp.concatenate([high, mid, low])
    extra = -(-parts.shape[0] // 16) * 16
    parts = jnp.pad(parts, (0, extra - parts.shape[0]))
    width = state.shape[1]
    packed = jnp.concatenate(
        [state.astype(bf16), jnp.broadcast_to(parts[:, None], (extra, width)).astype(bf16)], axis=0
    )
    everything = lax.all_gather(packed, SP)
    count = everything.shape[0]
    logs = everything[:, state.shape[0] : state.shape[0] + 3 * heads, 0].astype(f32)
    logs = logs.reshape(count, 3, heads).sum(axis=1)
    index = jnp.arange(count)
    between = (index[None, :] > index[:, None]) & (index[None, :] < here)
    reach = jnp.sum(jnp.where(between[:, :, None], logs[None], 0.0), axis=1)
    factor = jnp.where((index < here)[:, None], jnp.exp(reach), 0.0)
    states = everything[:, : state.shape[0]].reshape(count, heads, -1, width)
    return jnp.sum(factor[:, :, None, None] * states.astype(f32), axis=0)


def local(
    stream,
    queries,
    keys_in,
    values_in,
    gate_in,
    log_decay,
    head_gain,
    out_weight,
    norm_gain,
    gate_weight,
    up_weight,
    down_weight,
):
    gate_full, up_full, down_full = spread_weights(gate_weight, up_weight, down_weight)
    heads = log_decay.shape[1]
    dim = queries.shape[1] // heads
    running, total, within, state = retention(queries, keys_in, values_in, log_decay)
    incoming = incoming_states(total, state)
    mixed = []
    for h in range(heads):
        cut = slice(h * dim, (h + 1) * dim)
        carried = dot(queries[:, cut], incoming[h].astype(bf16))
        retained = within[h] + carried * jnp.exp(running[:, h])[:, None]
        center = jnp.mean(retained, axis=-1, keepdims=True)
        spread = jnp.mean(jnp.square(retained - center), axis=-1, keepdims=True)
        normed = (retained - center) * lax.rsqrt(spread + epsilon) * head_gain[cut].astype(f32)
        mixed.append((jax.nn.silu(gate_in[:, cut].astype(f32)) * normed).astype(bf16))
    terms = dot(jnp.concatenate(mixed, axis=1), out_weight)
    if lax.axis_size("tp") == 2:
        half = terms.shape[0] // 2
        terms = terms.astype(bf16)
        mine = lax.axis_index("tp") * half
        sent = swap(lax.dynamic_slice_in_dim(terms, half - mine, half, 0), "tp", 1)
        kept = lax.dynamic_slice_in_dim(terms, mine, half, 0)
        attended = kept.astype(f32) + sent.astype(f32)
    else:
        attended = scatter_pair(terms)
    residual = stream.astype(f32) + attended
    normed = (
        residual
        * lax.rsqrt(jnp.mean(residual * residual, axis=-1, keepdims=True) + epsilon)
        * norm_gain.astype(f32)
    ).astype(bf16)

    def block(rows):
        rows = gather_pair(rows)
        hidden = (jax.nn.silu(dot(rows, gate_full)) * dot(rows, up_full)).astype(bf16)
        return scatter_pair(dot(hidden, down_full))

    groups = lax.axis_size("far")
    result = residual
    arrived = [normed] + [swap(normed, "far", s) for s in range(1, groups)]
    for s in range(1, groups):
        result = result + swap(block(arrived[s]).astype(bf16), "far", s).astype(f32)
    result = result + block(arrived[0])
    return result.astype(bf16)


def solution(mesh):
    devices = mesh.devices
    count, pair = devices.shape
    split = Mesh(devices.reshape(GROUP, count // GROUP, pair), (*SP, "tp"))
    return jax.shard_map(
        local,
        mesh=split,
        in_specs=(
            P((*SP, "tp"), None),
            P(SP, "tp"),
            P(SP, "tp"),
            P(SP, "tp"),
            P(SP, "tp"),
            P(SP, "tp"),
            P("tp"),
            P("tp", None),
            P(),
            P(SP, "tp"),
            P(SP, "tp"),
            P("tp", SP),
        ),
        out_specs=P((*SP, "tp"), None),
        check_vma=False,
    )
```

```python
import jax
import jax.numpy as jnp
from jax import lax
from jax.sharding import Mesh, PartitionSpec as P

epsilon = 1e-06
GROUP = 4
SP = ("far", "near")
f32, bf16 = jnp.float32, jnp.bfloat16


def swap(value, axis, bits):
    size = lax.axis_size(axis)
    return lax.ppermute(value, axis, [(i, i ^ bits) for i in range(size)])


def near_blocks(value):
    size = lax.axis_size("near")
    steps = (1, 2) if size == 4 else range(1, size)
    return [value] + [swap(value, "near", s) for s in steps]


def near_rest(blocks):
    half = blocks[0].shape[0] // 2
    cut = [(block[:half], block[half:]) for block in blocks]
    if lax.axis_size("near") == 4:
        cut.append((swap(cut[1][0], "near", 2), swap(cut[2][1], "near", 1)))
    return cut


def spread_weights(gate_weight, up_weight, down_weight):
    groups = lax.axis_size("far")
    far_at = lax.axis_index("far")
    width = gate_weight.shape[1] // groups
    all_rows, all_columns = [], []
    for s in range(groups):
        at = (far_at ^ s) * width
        rows = jnp.concatenate(
            [
                lax.dynamic_slice_in_dim(gate_weight, at, width, 1),
                lax.dynamic_slice_in_dim(up_weight, at, width, 1),
            ],
            axis=0,
        )
        all_rows.append(swap(rows, "far", s) if s else rows)
    for s in range(groups):
        at = (far_at ^ s) * width
        all_columns.append(lax.dynamic_slice_in_dim(down_weight, at, width, 0))
    return [near_blocks(piece) for piece in all_rows], all_columns


def by_distance(value):
    groups, near = lax.axis_size("far"), lax.axis_size("near")
    here = lax.axis_index("far") * near + lax.axis_index("near")
    width = value.shape[1] // (groups * near)
    return jnp.concatenate(
        [
            lax.dynamic_slice_in_dim(value, (here ^ k) * width, width, 1)
            for k in range(groups * near)
        ],
        axis=1,
    )


def turned(value, bits):
    groups = lax.axis_size("far")
    width = value.shape[1] // groups
    return jnp.concatenate(
        [value[:, (g ^ bits) * width : ((g ^ bits) + 1) * width] for g in range(groups)], axis=1
    )


def gather_pair(rows):
    if lax.axis_size("tp") == 2:
        return jnp.concatenate([rows, swap(rows, "tp", 1)], axis=0)
    return lax.all_gather(rows, "tp", axis=0, tiled=True)


def scatter_pair(terms):
    terms = terms.astype(bf16)
    if lax.axis_size("tp") == 2:
        half = terms.shape[0] // 2
        return terms[:half].astype(f32) + swap(terms[half:], "tp", 1).astype(f32)
    return lax.psum_scatter(terms, "tp", scatter_dimension=0, tiled=True).astype(f32)


def dot(a, b, dims=((1,), (0,))):
    return lax.dot_general(a, b, (dims, ((), ())), preferred_element_type=f32)


def retention(queries, keys_in, values_in, log_decay):
    row_count, heads = log_decay.shape
    dim = queries.shape[1] // heads
    scale = dim ** (-0.5)
    running = jnp.cumsum(log_decay, axis=0)
    total = running[-1]
    offsets = jnp.arange(row_count)
    causal = offsets[:, None] >= offsets[None, :]
    within, states = [], []
    for h in range(heads):
        cut = slice(h * dim, (h + 1) * dim)
        q, k, v = queries[:, cut], keys_in[:, cut], values_in[:, cut]
        col = running[:, h]
        gap = jnp.minimum(col[:, None] - col[None, :], 0.0)
        table = jnp.where(causal, jnp.exp(gap), 0.0) * scale
        within.append(dot((dot(q, k, ((1,), (1,))) * table).astype(bf16), v))
        tail = (jnp.exp(total[h] - col) * scale)[:, None]
        states.append(dot((k.astype(f32) * tail).astype(bf16), v, ((0,), (0,))))
    return running, total, within, jnp.concatenate(states, axis=0)


def incoming_states(total, state, columns):
    heads = total.shape[0]
    near = lax.axis_size("near")
    here = lax.axis_index("far") * near + lax.axis_index("near")
    high = lax.reduce_precision(total, 8, 7)
    mid = lax.reduce_precision(total - high, 8, 7)
    low = total - high - mid
    parts = jnp.concatenate([high, mid, low])
    extra = -(-parts.shape[0] // 16) * 16
    parts = jnp.pad(parts, (0, extra - parts.shape[0]))
    width = state.shape[1]
    packed = jnp.concatenate(
        [state.astype(bf16), jnp.broadcast_to(parts[:, None], (extra, width)).astype(bf16)], axis=0
    )
    everything = lax.all_gather(packed, SP)
    everything, columns = lax.optimization_barrier((everything, columns))
    columns = [swap(piece, "far", s) if s else piece for s, piece in enumerate(columns)]
    count = everything.shape[0]
    logs = everything[:, state.shape[0] : state.shape[0] + 3 * heads, 0].astype(f32)
    logs = logs.reshape(count, 3, heads).sum(axis=1)
    index = jnp.arange(count)
    between = (index[None, :] > index[:, None]) & (index[None, :] < here)
    reach = jnp.sum(jnp.where(between[:, :, None], logs[None], 0.0), axis=1)
    factor = jnp.where((index < here)[:, None], jnp.exp(reach), 0.0)
    states = everything[:, : state.shape[0]].reshape(count, heads, -1, width)
    return jnp.sum(factor[:, :, None, None] * states.astype(f32), axis=0), columns


def local(
    stream,
    queries,
    keys_in,
    values_in,
    gate_in,
    log_decay,
    head_gain,
    out_weight,
    norm_gain,
    gate_weight,
    up_weight,
    down_weight,
):
    weight_rows, weight_columns = spread_weights(gate_weight, up_weight, down_weight)
    heads = log_decay.shape[1]
    dim = queries.shape[1] // heads
    running, total, within, state = retention(queries, keys_in, values_in, log_decay)
    incoming, weight_columns = incoming_states(total, state, weight_columns)
    mixed = []
    for h in range(heads):
        cut = slice(h * dim, (h + 1) * dim)
        carried = dot(queries[:, cut], incoming[h].astype(bf16))
        retained = within[h] + carried * jnp.exp(running[:, h])[:, None]
        center = jnp.mean(retained, axis=-1, keepdims=True)
        spread = jnp.mean(jnp.square(retained - center), axis=-1, keepdims=True)
        normed = (retained - center) * lax.rsqrt(spread + epsilon) * head_gain[cut].astype(f32)
        mixed.append((jax.nn.silu(gate_in[:, cut].astype(f32)) * normed).astype(bf16))
    terms = dot(jnp.concatenate(mixed, axis=1), out_weight).astype(bf16)
    if lax.axis_size("tp") == 2:
        half = terms.shape[0] // 2
        mine = lax.axis_index("tp") * half
        sent = swap(lax.dynamic_slice_in_dim(terms, half - mine, half, 0), "tp", 1)
        kept = lax.dynamic_slice_in_dim(terms, mine, half, 0)
        attended = kept.astype(f32) + sent.astype(f32)
    else:
        attended = scatter_pair(terms)
    residual = stream.astype(f32) + attended
    normed = (
        residual
        * lax.rsqrt(jnp.mean(residual * residual, axis=-1, keepdims=True) + epsilon)
        * norm_gain.astype(f32)
    ).astype(bf16)

    normed = by_distance(normed)
    normed, weight_rows, weight_columns = lax.optimization_barrier(
        (normed, weight_rows, weight_columns)
    )
    weight_rows = [block for piece in weight_rows for block in near_rest(piece)]
    weight_columns = [
        block for piece in weight_columns for block in near_rest(near_blocks(piece))
    ]
    groups = lax.axis_size("far")
    arrived = [normed] + [swap(normed, "far", s) for s in range(1, groups)]
    rows = [turned(gather_pair(piece), s) for s, piece in enumerate(arrived)]
    gate_full = jnp.concatenate([gate for gate, _ in weight_rows], axis=0)
    up_full = jnp.concatenate([up for _, up in weight_rows], axis=0)
    down_full = jnp.concatenate(
        [jnp.concatenate([part[i] for part in weight_columns], axis=1) for i in range(2)], axis=0
    )
    together = jnp.concatenate(rows, axis=0)
    hidden = (jax.nn.silu(dot(together, gate_full)) * dot(together, up_full)).astype(bf16)
    height = rows[0].shape[0]
    mixer_out = 0.0
    for s in (*range(1, groups), 0):
        part = scatter_pair(dot(hidden[s * height : (s + 1) * height], down_full))
        if s:
            part = turned(swap(part.astype(bf16), "far", s).astype(f32), s)
        mixer_out = mixer_out + part
    return (residual + by_distance(mixer_out)).astype(bf16)


def solution(mesh):
    devices = mesh.devices
    count, pair = devices.shape
    split = Mesh(devices.reshape(GROUP, count // GROUP, pair), (*SP, "tp"))
    return jax.shard_map(
        local,
        mesh=split,
        in_specs=(
            P((*SP, "tp"), None),
            P(SP, "tp"),
            P(SP, "tp"),
            P(SP, "tp"),
            P(SP, "tp"),
            P(SP, "tp"),
            P("tp"),
            P("tp", None),
            P(),
            P(SP, "tp"),
            P(SP, "tp"),
            P("tp", SP),
        ),
        out_specs=P((*SP, "tp"), None),
        check_vma=False,
    )
```
